32 devices in a mesh: ep: 32 (over z, y, x, core).
Axes of the slice: x: 2, y: 2, z: 4, core: 2. Of those that a mesh axis runs over, the one named last changes fastest.
Arguments:
- tokens: bfloat16 [512, 2048], P('ep'), may hold values from -6 to 6
- cache_keys: bfloat16 [512, 1024, 128], P('ep'), may hold values from -6 to 6
- cache_values: bfloat16 [512, 1024, 128], P('ep'), may hold values from -6 to 6
- cache_len: int32 [512], P('ep'), may hold values from 1 to 1024
- norm_gain_first: float32 [2048], replicated, may hold values from 0.1 to 1.9
- w_query: bfloat16 [2048, 2048], P(None, 'ep'), may hold values from -0.125 to 0.125
- w_key: bfloat16 [2048, 128], replicated, may hold values from -0.125 to 0.125
- w_value: bfloat16 [2048, 128], replicated, may hold values from -0.125 to 0.125
- head_bias: float32 [32], replicated, may hold values from -8.5 to -3
- w_output: bfloat16 [2048, 2048], P(None, 'ep'), may hold values from -0.125 to 0.125
- norm_gain_second: float32 [2048], replicated, may hold values from 0.1 to 1.9
- group_id: int32 [512], P('ep'), may hold values from 0 to 1, as said below
- member: int32 [512, 6], P('ep'), may hold values from 0 to 15, as said below
- group_gate: float32 [512], P('ep'), may hold values from 0.3 to 1
- member_weight: float32 [512, 6], P('ep'), may hold values from 0.05 to 0.5
- expert_gate_w: bfloat16 [32, 2048, 512], P('ep'), may hold values from -0.125 to 0.125
- expert_up_w: bfloat16 [32, 2048, 512], P('ep'), may hold values from -0.125 to 0.125
- expert_down_w: bfloat16 [32, 512, 2048], P('ep'), may hold values from -0.25 to 0.25
- dense_gate_w: bfloat16 [2048, 2048], P(None, 'ep'), may hold values from -0.125 to 0.125
- dense_up_w: bfloat16 [2048, 2048], P(None, 'ep'), may hold values from -1 to 1
- hidden_gain: float32 [2048], replicated, may hold values from 0.1 to 1.9
- dense_down_w: bfloat16 [2048, 2048], P(None, 'ep'), may hold values from -0.125 to 0.125
- branch_logit: float32 [2048], replicated, may hold values from -8 to 8
Outputs:
- mixed_out: bfloat16 [512, 2048], P('ep')
- new_keys: bfloat16 [512, 128], P('ep')
- new_values: bfloat16 [512, 128], P('ep')
The draws below stay inside these ranges and needn't reach their ends.
Inputs may be any that keep to these rules, and one draw needn't show every extreme that they name: `group_id`: each group number is named by exactly 8 of the tokens of one device. `member`: each row names 6 different members; with group_id, no expert is named by more than 8 tokens of one device, and some expert is named by 8 tokens of every device.
All inputs are finite; a program needn't handle non-finite values.
Results may differ from the reference program's by a relative error of at most 0.0085.
Values may be sent and summed in bfloat16 or wider, within the bound.
No kernel may reach another device: no remote copies, remote signals or barrier semaphores. Data moves between devices by JAX's collectives and lax.ppermute only.
A program may use at most 128 MiB of HBM per device.

```python
import math
import jax
import jax.numpy as jnp
from jax import lax

D = 2048
HEADS = 32
HEAD_DIM = 64
KV_HEADS = 2
FD = 2048
FE = 512
PER_GROUP = 16
TOP_K = 6
SEQ_DEV = 16
CACHE = 1024
TOKENS = 512
EXPERTS = 32
GROUPS = 2
N_EP = 32


def group_table(key):
    block_count = TOKENS // SEQ_DEV
    block_keys = jax.random.split(jax.random.fold_in(key, 11), block_count)

    def shuffle_block(block_key):
        return jax.random.permutation(block_key, SEQ_DEV)
    shuffled = jax.vmap(shuffle_block)(block_keys)
    return (shuffled % GROUPS).reshape(TOKENS).astype(jnp.int32)


def draw_group_id(key, part):
    return group_table(key)


def draw_member(key, part):
    groups_of = group_table(key)
    common = jax.random.randint(jax.random.fold_in(key, 12), (GROUPS,), 0, PER_GROUP)
    common_token = jnp.take(common, groups_of)
    columns = jnp.arange(PER_GROUP, dtype=jnp.int32)[None, :]
    scores = jax.random.randint(jax.random.fold_in(key, 13), (TOKENS, PER_GROUP), 0, 1 << 20) * PER_GROUP + columns
    scores = jnp.where(columns == common_token[:, None], 1 << 26, scores)
    unused, chosen = lax.top_k(scores, TOP_K)
    order_scores = jax.random.randint(jax.random.fold_in(key, 14), (TOKENS, TOP_K), 0, 1 << 20) * TOP_K
    order_scores = order_scores + jnp.arange(TOP_K, dtype=jnp.int32)[None, :]
    reorder = jnp.argsort(order_scores, axis=1)
    return jnp.take_along_axis(chosen, reorder, axis=1).astype(jnp.int32)


def draw_head_bias(key, part):
    return jax.random.uniform(key, (HEADS,), jnp.float32, -7.5, -3.0)


def draw_dense_up_w(key, part):
    base = jax.random.normal(jax.random.fold_in(key, 21), (D, FD), jnp.float32) * D ** (-0.5)
    ramp = jnp.arange(FD, dtype=jnp.float32) / FD
    rising = jnp.exp(ramp * math.log(4.0))
    rough = jnp.exp(jax.random.uniform(jax.random.fold_in(key, 22), (FD,), jnp.float32, -0.7, 0.7))
    scaled = jnp.clip(base * (rising * rough)[None, :], -1.0, 1.0)
    return scaled.astype(jnp.bfloat16)


def place_ends(array, rng, low, top_value):
    place = [jax.random.randint(jax.random.fold_in(rng, axis), (), 0, length) for axis, length in enumerate(array.shape)]
    main_axis = array.shape.index(max(array.shape))
    neighbour = place[:main_axis] + [(place[main_axis] + 1) % array.shape[main_axis]] + place[main_axis + 1:]
    return array.at[tuple(place)].set(low).at[tuple(neighbour)].set(top_value)


def block_levels(own_key, extent, shards, least, high):
    gain = 1.0
    for axis_at, parts in shards:
        steps = jax.random.uniform(jax.random.fold_in(jax.random.fold_in(own_key, 6), axis_at), (parts,), jnp.float32, least / len(shards), high / len(shards))
        gain = gain * jnp.repeat(jnp.exp(steps), extent[axis_at] // parts).reshape((-1,) + (1,) * (len(extent) - 1 - axis_at))
    return gain


def bell_draw(key, dims, scale, most, pieces=(), kind=jnp.bfloat16):
    loudness = block_levels(key, dims, pieces, -0.22, 0.18) if pieces else 1.0
    values = jax.random.normal(key, dims, jnp.float32) * scale * loudness
    return jnp.minimum(jnp.maximum(values, -most), most).astype(kind)


def setup_inputs(seed: int = 0) -> dict:
    seeds = jax.random.split(jax.random.key(seed), 24)
    tokens = bell_draw(seeds[0], (TOKENS, D), 1.0, 6.0, ((0, 32),))
    cache_keys = bell_draw(seeds[1], (TOKENS, CACHE, KV_HEADS * HEAD_DIM), 1.0, 6.0, ((0, 32),))
    cache_values = bell_draw(seeds[2], (TOKENS, CACHE, KV_HEADS * HEAD_DIM), 1.0, 6.0, ((0, 32),))
    cache_len = place_ends(jax.random.randint(seeds[3], (TOKENS,), 1, CACHE + 1), jax.random.fold_in(seeds[3], 1), 1, CACHE).astype(jnp.int32)
    norm_gain_first = jnp.clip(1.0 + 0.18 * jax.random.normal(seeds[4], (D,), jnp.float32), 0.1, 1.9)
    w_query = bell_draw(seeds[5], (D, HEADS * HEAD_DIM), D ** -0.5, 0.125, ((1, 32),))
    w_key = bell_draw(seeds[6], (D, KV_HEADS * HEAD_DIM), D ** -0.5, 0.125)
    w_value = bell_draw(seeds[7], (D, KV_HEADS * HEAD_DIM), D ** -0.5, 0.125)
    head_bias = draw_head_bias(jax.random.fold_in(seeds[23], 71), 0)
    w_output = bell_draw(seeds[9], (HEADS * HEAD_DIM, D), (HEADS * HEAD_DIM) ** -0.5, 0.125, ((1, 32),))
    norm_gain_second = jnp.clip(1.0 + 0.18 * jax.random.normal(seeds[10], (D,), jnp.float32), 0.1, 1.9)
    group_id = draw_group_id(jax.random.fold_in(seeds[23], 71), 0)
    member = draw_member(jax.random.fold_in(seeds[23], 71), 0)
    group_gate = jnp.clip(jnp.exp(math.log(1.0) - 1.2039728 * jax.random.uniform(seeds[13], (TOKENS,), jnp.float32) ** block_levels(seeds[13], (TOKENS,), ((0, 32),), -0.2, 0.2)), 0.3, 1.0)
    member_weight = jnp.clip(jnp.exp(math.log(0.5) - 2.3025851 * jax.random.uniform(seeds[14], (TOKENS, TOP_K), jnp.float32) ** block_levels(seeds[14], (TOKENS, TOP_K), ((0, 32),), -0.2, 0.2)), 0.05, 0.5)
    expert_gate_w = bell_draw(seeds[15], (EXPERTS, D, FE), D ** -0.5, 0.125, ((0, 32),))
    expert_up_w = bell_draw(seeds[16], (EXPERTS, D, FE), D ** -0.5, 0.125, ((0, 32),))
    expert_down_w = bell_draw(seeds[17], (EXPERTS, FE, D), FE ** -0.5, 0.25, ((0, 32),))
    dense_gate_w = bell_draw(seeds[18], (D, FD), D ** -0.5, 0.125, ((1, 32),))
    dense_up_w = draw_dense_up_w(jax.random.fold_in(seeds[23], 71), 0)
    hidden_gain = jnp.clip(1.0 + 0.18 * jax.random.normal(seeds[20], (FD,), jnp.float32), 0.1, 1.9)
    dense_down_w = bell_draw(seeds[21], (FD, D), FD ** -0.5, 0.125, ((1, 32),))
    branch_logit = bell_draw(seeds[22], (D,), 1.5, 8.0, (), jnp.float32)
    return {"tokens": tokens, "cache_keys": cache_keys, "cache_values": cache_values, "cache_len": cache_len, "norm_gain_first": norm_gain_first, "w_query": w_query, "w_key": w_key, "w_value": w_value, "head_bias": head_bias, "w_output": w_output, "norm_gain_second": norm_gain_second, "group_id": group_id, "member": member, "group_gate": group_gate, "member_weight": member_weight, "expert_gate_w": expert_gate_w, "expert_up_w": expert_up_w, "expert_down_w": expert_down_w, "dense_gate_w": dense_gate_w, "dense_up_w": dense_up_w, "hidden_gain": hidden_gain, "dense_down_w": dense_down_w, "branch_logit": branch_logit}


epsilon = 1e-06
pair_block = 32

def rms_scale(values):
    return lax.rsqrt(lax.optimization_barrier(jnp.mean(values * values, axis=-1, keepdims=True)) + epsilon)

def stick_read(queries, key_cache, value_cache, lengths, head_bias):
    batch_size = queries.shape[0]
    span_len = key_cache.shape[1]
    group_size = HEADS // KV_HEADS
    query_heads = queries.reshape(batch_size, KV_HEADS, group_size, HEAD_DIM).astype(jnp.float32)
    key_heads = key_cache.reshape(batch_size, span_len, KV_HEADS, HEAD_DIM).astype(jnp.float32)
    value_heads = value_cache.reshape(batch_size, span_len, KV_HEADS, HEAD_DIM).astype(jnp.float32)
    scores = jnp.einsum('bkgd,bskd->bkgs', query_heads, key_heads) * HEAD_DIM ** (-0.5)
    scores = scores + head_bias.reshape(KV_HEADS, group_size)[None, :, :, None]
    live_mask = (jnp.arange(span_len, dtype=jnp.int32)[None, :] < lengths[:, None])[:, None, None, :]
    log_remain = jnp.where(live_mask, jax.nn.log_sigmoid(-scores), 0.0)
    remain_after = lax.cumsum(log_remain, axis=3, reverse=True) - log_remain
    weights = jnp.where(live_mask, jnp.exp(jax.nn.log_sigmoid(scores) + remain_after), 0.0).astype(jnp.bfloat16)
    mixed_heads = jnp.einsum('bkgs,bskd->bkgd', weights.astype(jnp.float32), value_heads)
    return mixed_heads.reshape(batch_size, HEADS * HEAD_DIM).astype(jnp.bfloat16)

def expert_apply(expert, pair_rows, expert_gate_w, expert_up_w, expert_down_w):
    gate_w = lax.dynamic_index_in_dim(expert_gate_w, expert, 0, keepdims=False)
    up_w = lax.dynamic_index_in_dim(expert_up_w, expert, 0, keepdims=False)
    down_w = lax.dynamic_index_in_dim(expert_down_w, expert, 0, keepdims=False)
    gate_pre = jnp.dot(pair_rows, gate_w, preferred_element_type=jnp.float32)
    upper_pre = jnp.dot(pair_rows, up_w, preferred_element_type=jnp.float32)
    hidden = (jax.nn.silu(gate_pre) * upper_pre).astype(jnp.bfloat16)
    return jnp.dot(hidden, down_w, preferred_element_type=jnp.float32).astype(jnp.bfloat16)

def reference(tokens, cache_keys, cache_values, cache_len, norm_gain_first, w_query, w_key, w_value, head_bias, w_output, norm_gain_second, group_id, member, group_gate, member_weight, expert_gate_w, expert_up_w, expert_down_w, dense_gate_w, dense_up_w, hidden_gain, dense_down_w, branch_logit):
    stream = tokens.astype(jnp.float32)
    normed_first = (stream * rms_scale(stream) * norm_gain_first).astype(jnp.bfloat16)
    queries = jnp.dot(normed_first, w_query, preferred_element_type=jnp.float32).astype(jnp.bfloat16)
    new_keys = jnp.dot(normed_first, w_key, preferred_element_type=jnp.float32).astype(jnp.bfloat16)
    new_values = jnp.dot(normed_first, w_value, preferred_element_type=jnp.float32).astype(jnp.bfloat16)

    def attend_block(block_args):
        block_queries, block_keys, block_values, block_lens = block_args
        return stick_read(block_queries, block_keys, block_values, block_lens, head_bias)
    attended = lax.map(attend_block, (queries.reshape(N_EP, SEQ_DEV, HEADS * HEAD_DIM), cache_keys.reshape(N_EP, SEQ_DEV, CACHE, KV_HEADS * HEAD_DIM), cache_values.reshape(N_EP, SEQ_DEV, CACHE, KV_HEADS * HEAD_DIM), cache_len.reshape(N_EP, SEQ_DEV))).reshape(TOKENS, HEADS * HEAD_DIM)
    projected = jnp.dot(attended, w_output, preferred_element_type=jnp.float32).astype(jnp.bfloat16)
    second_stream = stream + projected.astype(jnp.float32)
    normed_second = (second_stream * rms_scale(second_stream) * norm_gain_second).astype(jnp.bfloat16)
    pair_expert = (group_id[:, None] * PER_GROUP + member).reshape(-1).astype(jnp.int32)
    pair_total = pair_expert.shape[0]
    sort_order = jnp.argsort(pair_expert, stable=True).astype(jnp.int32)
    sorted_expert = pair_expert[sort_order]
    pair_rows = normed_second[sort_order // TOP_K]

    def run_block(block_index):
        block_rows = lax.dynamic_slice_in_dim(pair_rows, block_index * pair_block, pair_block, 0)
        block_expert = lax.dynamic_slice_in_dim(sorted_expert, block_index * pair_block, pair_block, 0)

        def visit(expert, accum):
            result_rows = expert_apply(expert, block_rows, expert_gate_w, expert_up_w, expert_down_w)
            return jnp.where((block_expert == expert)[:, None], result_rows.astype(jnp.float32), accum)
        return lax.fori_loop(block_expert[0], block_expert[pair_block - 1] + 1, visit, jnp.zeros((pair_block, D), jnp.float32))
    sorted_out = lax.map(run_block, jnp.arange(pair_total // pair_block, dtype=jnp.int32)).reshape(pair_total, D)
    expert_out = jnp.zeros((pair_total, D), jnp.float32).at[sort_order].set(sorted_out)
    combine = group_gate[:, None] * member_weight
    routed = lax.optimization_barrier(jnp.sum(expert_out.reshape(TOKENS, TOP_K, D) * combine[:, :, None], axis=1))
    dense_gate = jnp.dot(normed_second, dense_gate_w, preferred_element_type=jnp.float32)
    dense_upper = jnp.dot(normed_second, dense_up_w, preferred_element_type=jnp.float32)
    dense_hidden = jax.nn.silu(dense_gate) * dense_upper
    dense_normed = (dense_hidden * rms_scale(dense_hidden) * hidden_gain).astype(jnp.bfloat16)
    dense_out = jnp.dot(dense_normed, dense_down_w, preferred_element_type=jnp.float32).astype(jnp.bfloat16)
    mixed_out = second_stream + routed + jax.nn.sigmoid(branch_logit) * dense_out.astype(jnp.float32)
    return (mixed_out.astype(jnp.bfloat16), new_keys, new_values)
```

```python
import jax
import jax.numpy as jnp
from jax import lax
from jax.sharding import PartitionSpec as P

D = 2048
HEADS = 32
HEAD_DIM = 64
KV_HEADS = 2
PER_GROUP = 16


epsilon = 1e-06


def rms_scale(values):
    return lax.rsqrt(jnp.mean(values * values, axis=-1, keepdims=True) + epsilon)


def later_sum(log_remain):
    span_len = log_remain.shape[-1]
    block_len = min(128, span_len)
    block_count = span_len // block_len
    lead = log_remain.shape[:-1]
    blocked = log_remain.reshape(lead + (block_count, block_len))
    inner = jnp.arange(block_len, dtype=jnp.int32)
    inner_after = (inner[:, None] > inner[None, :]).astype(jnp.float32)
    within = jnp.einsum("abcnj,js->abcns", blocked, inner_after, precision=lax.Precision.HIGHEST)
    totals = jnp.sum(blocked, axis=-1)
    outer = jnp.arange(block_count, dtype=jnp.int32)
    outer_after = (outer[:, None] > outer[None, :]).astype(jnp.float32)
    carried = jnp.einsum("abcj,jn->abcn", totals, outer_after, precision=lax.Precision.HIGHEST)
    return (within + carried[..., None]).reshape(lead + (span_len,))


def stick_scores(queries, key_cache, lengths, head_bias):
    batch_size = queries.shape[0]
    span_len = key_cache.shape[1]
    group_size = HEADS // KV_HEADS
    query_heads = queries.reshape(batch_size, KV_HEADS, group_size, HEAD_DIM)
    key_heads = key_cache.reshape(batch_size, span_len, KV_HEADS, HEAD_DIM)
    scores = jnp.einsum(
        "bkgd,bskd->bkgs", query_heads, key_heads, preferred_element_type=jnp.float32
    ) * HEAD_DIM ** (-0.5)
    scores = scores + head_bias.reshape(KV_HEADS, group_size)[None, :, :, None]
    live_mask = (jnp.arange(span_len, dtype=jnp.int32)[None, :] < lengths[:, None])[
        :, None, None, :
    ]
    log_remain = jnp.where(live_mask, jax.nn.log_sigmoid(-scores), 0.0)
    remain_after = later_sum(log_remain)
    weights = jnp.where(live_mask, jnp.exp(jax.nn.log_sigmoid(scores) + remain_after), 0.0).astype(
        jnp.bfloat16
    )
    return weights


def stick_read(weights, value_cache):
    batch_size, span_len = value_cache.shape[:2]
    value_heads = value_cache.reshape(batch_size, span_len, KV_HEADS, HEAD_DIM)
    mixed_heads = jnp.einsum(
        "bkgs,bskd->bkgd", weights, value_heads, preferred_element_type=jnp.float32
    )
    return mixed_heads.reshape(batch_size, HEADS * HEAD_DIM).astype(jnp.bfloat16)


def exchange(values, offset):
    devices = lax.axis_size("ep")
    return lax.ppermute(values, "ep", [(i, i ^ offset) for i in range(devices)])


def gather_rows(values, offsets):
    blocks = values[None]
    for offset in offsets:
        blocks = jnp.concatenate([blocks, exchange(blocks, offset)], axis=0)
    return blocks


def scatter_blocks(blocks, offsets):
    blocks = blocks[:, None]
    for j in reversed(range(len(offsets))):
        pairs = blocks.reshape((2, 1 << j) + blocks.shape[1:])
        blocks = jnp.concatenate([pairs[0], exchange(pairs[1], offsets[j])], axis=1)
    return blocks[0]


def reduce_blocks(blocks, offsets):
    for j in reversed(range(len(offsets))):
        pairs = blocks.reshape((2, 1 << j) + blocks.shape[1:])
        sent = exchange(pairs[1].astype(jnp.bfloat16), offsets[j])
        blocks = pairs[0] + sent.astype(jnp.float32)
    return blocks[0]


def source_offsets(offsets):
    count = len(offsets)
    return [
        sum(offsets[count - 1 - bit] for bit in range(count) if s >> bit & 1)
        for s in range(1 << count)
    ]


def gather_columns(transposed, offsets):
    return jnp.concatenate([transposed] + [exchange(transposed, o) for o in offsets], axis=0)


def dot_nt(left, right):
    return lax.dot_general(
        left, right, (((1,), (1,)), ((), ())), preferred_element_type=jnp.float32
    )


def project(rows, columns, near, far, me):
    seq_dev = rows.shape[0]
    gathered = gather_rows(rows, near)
    mixed = dot_nt(gathered.reshape(-1, rows.shape[1]), columns).astype(jnp.bfloat16)
    own = scatter_blocks(mixed.reshape(len(gathered), seq_dev, -1), near)
    spans = len(far) + 1
    own = own.reshape(own.shape[0], seq_dev, spans, -1)
    slots = jnp.array([[s ^ f for f in [0] + far] for s in source_offsets(near)], jnp.int32)
    total = slots.size
    place = (jnp.arange(total, dtype=jnp.int32)[:, None, None] == (slots ^ me)[None]).astype(
        jnp.bfloat16
    )
    whole = jnp.einsum("hsr,sbrd->bhd", place, own, preferred_element_type=jnp.float32)
    return whole.astype(jnp.bfloat16).reshape(seq_dev, -1)


def shards(
    tokens,
    cache_keys,
    cache_values,
    cache_len,
    norm_gain_first,
    w_query,
    w_key,
    w_value,
    head_bias,
    w_output,
    norm_gain_second,
    group_id,
    member,
    group_gate,
    member_weight,
    expert_gate_w,
    expert_up_w,
    expert_down_w,
    dense_gate_w,
    dense_up_w,
    hidden_gain,
    dense_down_w,
    branch_logit,
):
    devices = lax.axis_size("ep")
    me = lax.axis_index("ep")
    seq_dev = tokens.shape[0]
    groups = devices // PER_GROUP
    capacity = seq_dev // groups
    group = me // PER_GROUP
    place_in = me % PER_GROUP
    near = [4, 2, 1]
    far = [8 * i for i in range(1, devices // 8)]
    inside = [8, 4, 2, 1]
    across = [PER_GROUP << i for i in range((groups - 1).bit_length())]
    other = [PER_GROUP * i for i in range(1, groups)]

    query_cols = gather_columns(w_query.T, far)
    stream = tokens.astype(jnp.float32)
    normed_first = (stream * rms_scale(stream) * norm_gain_first).astype(jnp.bfloat16)
    new_keys = jnp.dot(normed_first, w_key, preferred_element_type=jnp.float32).astype(jnp.bfloat16)
    new_values = jnp.dot(normed_first, w_value, preferred_element_type=jnp.float32).astype(
        jnp.bfloat16
    )
    queries = project(normed_first, query_cols, near, far, me)

    output_cols = gather_columns(w_output.T, far)
    gate_cols = gather_columns(dense_gate_w.T, other)
    up_cols = gather_columns(dense_up_w.T, other)
    width = dense_down_w.shape[1]
    down_parts = dense_down_w.reshape(groups, PER_GROUP, width, width)
    down_parts = jnp.concatenate(
        [
            lax.dynamic_index_in_dim(down_parts, group ^ r, 0, keepdims=False)
            for r in range(groups)
        ],
        axis=1,
    )
    members = [[g * PER_GROUP + m for m in range(PER_GROUP)] for g in range(groups)]
    down_own = lax.all_to_all(
        down_parts, "ep", split_axis=0, concat_axis=0, tiled=True, axis_index_groups=members
    )
    down_own = down_own.transpose(1, 0, 2).reshape(groups * width, PER_GROUP * width)
    spans = [down_own] + [exchange(down_own, o) for o in other]
    down_rel = jnp.stack(
        [
            jnp.concatenate(
                [lax.slice_in_dim(s, (r ^ q) * width, ((r ^ q) + 1) * width) for q in range(groups)]
            )
            for r, s in enumerate(spans)
        ]
    )
    down_rows = jnp.concatenate(
        [
            lax.dynamic_index_in_dim(down_rel, group ^ r, 0, keepdims=False)
            for r in range(groups)
        ],
        axis=1,
    )
    gains = hidden_gain.reshape(groups, PER_GROUP, width)
    own_gain = jnp.concatenate(
        [
            lax.dynamic_slice(gains, (group ^ r, place_in, 0), (1, 1, width)).reshape(width)
            for r in range(groups)
        ]
    )

    stick_weights = stick_scores(queries, cache_keys, cache_len, head_bias)
    attended = stick_read(stick_weights, cache_values)
    projected = project(attended, output_cols, near, far, me)
    second_stream = stream + projected.astype(jnp.float32)
    normed_second = (second_stream * rms_scale(second_stream) * norm_gain_second).astype(
        jnp.bfloat16
    )

    order = jnp.arange(seq_dev, dtype=jnp.int32)
    same = group_id[:, None] == group_id[None, :]
    rank = jnp.sum((same & (order[None, :] < order[:, None])).astype(jnp.int32), axis=1)
    slot = (group_id ^ group) * capacity + rank
    select = (jnp.arange(groups * capacity, dtype=jnp.int32)[:, None] == slot[None, :]).astype(
        jnp.bfloat16
    )
    chosen = member[:, :, None] == jnp.arange(PER_GROUP, dtype=jnp.int32)[None, None, :]
    share = jnp.sum(
        jnp.where(chosen, (group_gate[:, None] * member_weight)[:, :, None], 0.0), axis=1
    )
    share_high = lax.reduce_precision(share, 8, 7)
    share_low = share - share_high
    extra = jnp.concatenate(
        [share_high, share_low, jnp.zeros((seq_dev, 128 - 2 * PER_GROUP), jnp.float32)], axis=1
    ).astype(jnp.bfloat16)
    packed = jnp.dot(
        select,
        jnp.concatenate([normed_second, extra], axis=1),
        preferred_element_type=jnp.float32,
    ).astype(jnp.bfloat16)
    packed = scatter_blocks(packed.reshape(groups, capacity, -1), across)
    arrived = gather_rows(packed.reshape(groups * capacity, -1), inside)
    arrived = arrived.reshape(-1, arrived.shape[-1])
    rows = arrived[:, :D]
    shares = arrived[:, D:].astype(jnp.float32)
    column = jnp.arange(shares.shape[1], dtype=jnp.int32)
    mine = (column == place_in) | (column == place_in + PER_GROUP)
    weight = jnp.sum(jnp.where(mine[None, :], shares, 0.0), axis=1, keepdims=True)

    dense_hidden = jax.nn.silu(dot_nt(rows, gate_cols)) * dot_nt(rows, up_cols)
    squares = jnp.sum(dense_hidden * dense_hidden, axis=1)
    squares = squares.reshape(PER_GROUP, groups * capacity)
    for j, offset in enumerate(inside):
        peer = exchange(squares, offset).reshape(-1, 2, 1 << j, groups * capacity)
        squares = squares + peer[:, ::-1].reshape(squares.shape)
    squares = squares.reshape(-1)
    scale = lax.rsqrt(squares / hidden_gain.shape[0] + epsilon)
    dense_part = jnp.dot(
        (dense_hidden * own_gain).astype(jnp.bfloat16),
        down_rows,
        preferred_element_type=jnp.float32,
    )
    gate_pre = jnp.dot(rows, expert_gate_w[0], preferred_element_type=jnp.float32)
    upper_pre = jnp.dot(rows, expert_up_w[0], preferred_element_type=jnp.float32)
    hidden = (jax.nn.silu(gate_pre) * upper_pre).astype(jnp.bfloat16)
    expert_out = jnp.dot(hidden, expert_down_w[0], preferred_element_type=jnp.float32)
    partial = expert_out * weight + dense_part * scale[:, None] * jax.nn.sigmoid(branch_logit)
    summed = reduce_blocks(
        partial.reshape(len(arrived) // (groups * capacity), groups, capacity, D), inside
    )
    returned = scatter_blocks(summed.astype(jnp.bfloat16), across[::-1])
    branches = lax.dot_general(
        select,
        returned.reshape(groups * capacity, D),
        (((0,), (0,)), ((), ())),
        preferred_element_type=jnp.float32,
    )
    mixed_out = second_stream + branches
    return (mixed_out.astype(jnp.bfloat16), new_keys, new_values)


def solution(mesh):
    in_specs = (
        P("ep", None),
        P("ep", None, None),
        P("ep", None, None),
        P("ep"),
        P(),
        P(None, "ep"),
        P(),
        P(),
        P(),
        P(None, "ep"),
        P(),
        P("ep"),
        P("ep", None),
        P("ep"),
        P("ep", None),
        P("ep", None, None),
        P("ep", None, None),
        P("ep", None, None),
        P(None, "ep"),
        P(None, "ep"),
        P(),
        P(None, "ep"),
        P(),
    )
    out_specs = (P("ep", None), P("ep", None), P("ep", None))
    return jax.shard_map(shards, mesh=mesh, in_specs=in_specs, out_specs=out_specs, check_vma=False)
```
